32 devices in a mesh: fs: 4 (over z), tp: 8 (over y, x, core).
Axes of the slice: x: 2, y: 2, z: 4, core: 2. Of those that a mesh axis runs over, the one named last changes fastest.
Arguments:
- tokens: bfloat16 [1024, 2048], P('fs', 'tp'), may hold values from -6 to 6
- norm_gain: float32 [2048], P('tp'), may hold values from 0.1 to 1.9
- gate_master: float32 [8, 3584, 2048], P(None, 'fs', 'tp'), may hold values from -0.125 to 0.125
- up_master: float32 [8, 3584, 2048], P(None, 'fs', 'tp'), may hold values from -0.125 to 0.125
- down_master: float32 [8, 3584, 2048], P(None, 'fs', 'tp'), may hold values from -0.0625 to 0.0625
- routes: int32 [1024, 2], P('fs'), may hold values from 0 to 3, all different within a row; in each aligned block of 256 rows (0 to 255, 256 to 511, ...) at most 128 rows name the same one
- route_logits: float32 [1024, 2], P('fs'), may hold values from -8 to 8
Outputs:
- gate_serve: bfloat16 [8, 3584, 2048], P('tp', 'fs')
- up_serve: bfloat16 [8, 3584, 2048], P('tp', 'fs')
- down_serve: bfloat16 [8, 3584, 2048], P('tp', 'fs')
- mixed_tokens: bfloat16 [1024, 2048], P('fs', 'tp')
The draws below stay inside these ranges and needn't reach their ends.
Inputs may be any that keep to these rules, and one draw needn't show every extreme that they name: `routes`: each row names 2 different experts; in every aligned block of 256 rows each expert is named by exactly 128 rows.
All inputs are finite; a program needn't handle non-finite values.
Results may differ from the reference program's by a relative error of at most 0.024.
Values may be sent and summed in bfloat16 or wider, within the bound.
No kernel may reach another device: no remote copies, remote signals or barrier semaphores. Data moves between devices by JAX's collectives and lax.ppermute only.
A program may use at most 128 MiB of HBM per device.

```python
import math
import jax
import jax.numpy as jnp
import numpy as np
from jax import lax

D = 2048
FF = 7168
TOP = 2
TOK_DEV = 256
EXPERTS = 4
SLABS = 8
FF_SLAB = 3584
TOKENS = 1024
CAP = 128
N_FS = 4


def block_levels(key, extent, pieces, low, top_value):
    def one(position, shards_of):
        steps = jax.random.uniform(jax.random.fold_in(jax.random.fold_in(key, 6), position), (shards_of,), jnp.float32, low / len(pieces), top_value / len(pieces))
        return jnp.repeat(jnp.exp(steps), extent[position] // shards_of).reshape((-1,) + (1,) * (len(extent) - position - 1))

    factor_of = one(*pieces[0])
    for cut in pieces[1:]:
        factor_of = factor_of * one(*cut)
    return factor_of


def assign_block(own_key, own, number, rows, number_of, top, bound, lean):
    order = jax.random.permutation(own_key, number_of)
    crowded, common = portions_of(number_of, rows * top, bound, lean, True), portions_of(number_of, rows * top, bound, lean, False)
    places = jnp.arange(number_of)

    def named(sizes, offset_by):
        used = int((sizes > 0).sum())
        fixed = max(1, used // 4)
        shifted = fixed + (places - fixed + offset_by * (used - fixed)) % max(1, number_of - fixed)
        return jnp.zeros((number_of,), jnp.int32).at[order[jnp.where(places < fixed, places, shifted)]].set(jnp.asarray(sizes, jnp.int32))

    sizes = jnp.where(number % 4 == 0, named(crowded, number // 4), named(common, number - number // 4 - 1))
    mixed = jax.random.permutation(jax.random.fold_in(own, 3), number_of)
    giver, sink = mixed[0:number_of // 2 * 2:2], mixed[1:number_of // 2 * 2:2]
    margin = jnp.minimum(sizes[giver] - 1, bound - sizes[sink]) // 2
    margin = jnp.where((giver == order[0]) | (sink == order[0]) | (sizes[sink] == 0), 0, jnp.maximum(margin, 0))
    shifted = jax.random.randint(jax.random.fold_in(own, 4), (number_of // 2,), 0, 1 << 20) % (margin + 1)
    sizes = sizes.at[giver].add(-shifted).at[sink].add(shifted)
    items = jnp.searchsorted(jnp.cumsum(sizes), jnp.arange(rows * top), side="right").astype(jnp.int32)
    grid = items.reshape(top, rows).T
    grid = grid[jax.random.permutation(jax.random.fold_in(own, 1), rows)]
    offset_by = jax.random.randint(jax.random.fold_in(own, 2), (rows, 1), 0, top)
    return jnp.take_along_axis(grid, (jnp.arange(top)[None, :] + offset_by) % top, axis=1)


def portions_of(number_of, total, limit, slope, full):
    weights = [(1 << 20) // math.isqrt(standing ** slope) + 1 for standing in range(1, number_of + 1)]
    largest = limit if full else min(limit, max(-(-total // number_of), total * weights[0] // sum(weights)))
    least = 1 if total - largest >= number_of - 1 else 0
    counts, spare = [largest] + [least] * (number_of - 1), total - largest - least * (number_of - 1)
    while spare > 0:
        candidates = [i for i in range(1, number_of) if counts[i] < largest] or [i for i in range(1, number_of) if counts[i] < limit]
        pool, left = sum([weights[i] for i in candidates]), spare
        for i in candidates:
            addition = min(limit - counts[i], max(1, left * weights[i] // pool), spare)
            counts[i] = counts[i] + addition
            spare = spare - addition
    return np.array(counts)


def normal_values(key, shape, width, limit, split=(), kind=jnp.bfloat16):
    drawn = width * jax.random.normal(key, shape, jnp.float32)
    if split:
        drawn = drawn * block_levels(key, shape, split, -0.22, 0.18)
    return jnp.clip(drawn, -limit, limit).astype(kind)


def setup_inputs(seed: int = 0) -> dict:
    seeds = jax.random.split(jax.random.key(seed), 8)
    tokens = normal_values(seeds[0], (TOKENS, D), 1.0, 6.0, ((0, 4), (1, 8)))
    norm_gain = jnp.clip(1.0 + 0.18 * jax.random.normal(seeds[1], (D,), jnp.float32), 0.1, 1.9)
    gate_master = normal_values(seeds[2], (SLABS, FF_SLAB, D), D ** -0.5, 0.125, ((1, 4), (2, 8)), jnp.float32)
    up_master = normal_values(seeds[3], (SLABS, FF_SLAB, D), D ** -0.5, 0.125, ((1, 4), (2, 8)), jnp.float32)
    down_master = normal_values(seeds[4], (SLABS, FF_SLAB, D), FF ** -0.5, 0.0625, ((1, 4), (2, 8)), jnp.float32)
    routes_keys = jax.random.split(jax.random.fold_in(seeds[5], 1), TOKENS // TOK_DEV)
    routes_turns = jax.random.permutation(jax.random.fold_in(seeds[5], 3), TOKENS // TOK_DEV)
    routes = jax.vmap(lambda own, number: assign_block(jax.random.fold_in(seeds[5], 2), own, number, TOK_DEV, EXPERTS, TOP, CAP, 0))(routes_keys, routes_turns).reshape((TOKENS, TOP))
    route_logits = normal_values(seeds[6], (TOKENS, TOP), 2.0, 8.0, ((0, 4),), jnp.float32)
    return dict(tokens=tokens, norm_gain=norm_gain, gate_master=gate_master, up_master=up_master, down_master=down_master, routes=routes, route_logits=route_logits)


epsilon = 1e-05

def reference(tokens, norm_gain, gate_master, up_master, down_master, routes, route_logits):
    gain_row = norm_gain[None, None, :]
    gate_serve = (gate_master * gain_row).astype(jnp.bfloat16)
    up_serve = (up_master * gain_row).astype(jnp.bfloat16)
    down_serve = down_master.astype(jnp.bfloat16)
    widened = tokens.astype(jnp.float32)
    row_scale = lax.rsqrt(lax.optimization_barrier(jnp.mean(widened * widened, axis=-1, keepdims=True)) + epsilon)
    normed = (widened * row_scale).astype(jnp.bfloat16)
    first_prob = jax.nn.sigmoid(route_logits[:, 0] - route_logits[:, 1])
    choice_prob = jnp.stack([first_prob, 1.0 - first_prob], axis=1)
    row_total = N_FS * CAP
    block_rows = FF_SLAB // N_FS

    def one_expert(expert_id):
        matches = routes == expert_id
        is_member = jnp.any(matches, axis=1)
        weight = lax.optimization_barrier(jnp.sum(jnp.where(matches, choice_prob, 0.0), axis=1))
        row_index = jnp.nonzero(is_member, size=row_total)[0].astype(jnp.int32)
        picked = normed[row_index]
        block_parts = jnp.zeros((N_FS, row_total, D), jnp.float32)
        for half_index in range(2):
            slab_id = 2 * expert_id + half_index
            gate_slab = lax.dynamic_index_in_dim(gate_serve, slab_id, 0, keepdims=False)
            up_slab = lax.dynamic_index_in_dim(up_serve, slab_id, 0, keepdims=False)
            down_slab = lax.dynamic_index_in_dim(down_serve, slab_id, 0, keepdims=False)
            gate_pre = jnp.dot(picked, gate_slab.T, preferred_element_type=jnp.float32)
            up_pre = jnp.dot(picked, up_slab.T, preferred_element_type=jnp.float32)
            hidden = (jax.nn.silu(gate_pre) * up_pre).astype(jnp.bfloat16)
            block_parts = block_parts + jnp.einsum('rfk,fkd->frd', hidden.reshape(row_total, N_FS, block_rows).astype(jnp.float32), down_slab.reshape(N_FS, block_rows, D).astype(jnp.float32))
        rounded = lax.optimization_barrier(block_parts.astype(jnp.bfloat16))
        expert_out = lax.optimization_barrier(jnp.sum(rounded.astype(jnp.float32), axis=0)).astype(jnp.bfloat16)
        return (row_index, weight[row_index][:, None] * expert_out.astype(jnp.float32))
    expert_ids = jnp.arange(EXPERTS, dtype=jnp.int32)
    all_index, all_terms = lax.map(one_expert, expert_ids)
    mixed = jnp.zeros((TOKENS, D), jnp.float32).at[all_index.reshape(-1)].add(all_terms.reshape(-1, D))
    return (gate_serve, up_serve, down_serve, mixed.astype(jnp.bfloat16))
```

```python
import functools

import jax
import jax.numpy as jnp
from jax import lax
from jax.experimental import pallas as pl
from jax.experimental.pallas import tpu as pltpu
from jax.sharding import PartitionSpec as P

epsilon = 1e-05


def swap(value, axis, mask, scope):
    if mask == 0:
        return value
    pairs = [(source, source ^ mask) for source in range(lax.axis_size(axis))]
    with jax.named_scope(scope):
        return lax.ppermute(value, axis, pairs)


def row_tile(rows):
    return 128 if rows % 128 == 0 else rows


def norm_kernel(me_ref, *refs):
    chunks, out_ref = refs[:-1], refs[-1]
    width = chunks[0].shape[1]
    total = jnp.zeros((chunks[0].shape[0], 1), jnp.float32)
    for ref in chunks:
        wide = ref[...].astype(jnp.float32)
        total = total + jnp.sum(wide * wide, axis=1, keepdims=True)
    scale = lax.rsqrt(total / (width * len(chunks)) + epsilon)
    for mask, ref in enumerate(chunks):
        start = pl.multiple_of((me_ref[0] ^ mask) * width, width)
        out_ref[:, pl.ds(start, width)] = (ref[...].astype(jnp.float32) * scale).astype(
            jnp.bfloat16
        )


def norm_rows(me, chunks):
    rows, width = chunks[0].shape
    return pl.pallas_call(
        norm_kernel,
        out_shape=jax.ShapeDtypeStruct((rows, width * len(chunks)), jnp.bfloat16),
        in_specs=[pl.BlockSpec(memory_space=pltpu.SMEM)]
        + [pl.BlockSpec(memory_space=pltpu.VMEM)] * len(chunks),
        out_specs=pl.BlockSpec(memory_space=pltpu.VMEM),
        cost_estimate=pl.CostEstimate(flops=10**8, bytes_accessed=10**6, transcendentals=0),
        name="norm_rows",
    )(me, *chunks)


contract = (((1,), (1,)), ((), ()))


def place(me_ref, pieces, slab_ref):
    width = pieces[0].shape[1]
    for mask, ref in enumerate(pieces):
        start = pl.multiple_of((me_ref[0] ^ mask) * width, width)
        slab_ref[0, :, pl.ds(start, width)] = ref[...]


def gate_kernel(count, me_ref, mine_ref, theirs_ref, *refs):
    pieces, (slab_ref, act_ref) = refs[:count], refs[count:]
    place(me_ref, pieces, slab_ref)
    half = mine_ref.shape[0]
    for number, rows in enumerate((mine_ref, theirs_ref)):
        pre = lax.dot_general(rows[...], slab_ref[0], contract, preferred_element_type=jnp.float32)
        act_ref[pl.ds(number * half, half), :] = pre * (1.0 / (1.0 + jnp.exp(-pre)))


def up_kernel(count, me_ref, mine_ref, theirs_ref, act_ref, *refs):
    pieces, (slab_ref, hidden_ref) = refs[:count], refs[count:]
    place(me_ref, pieces, slab_ref)
    half = mine_ref.shape[0]
    for number, rows in enumerate((mine_ref, theirs_ref)):
        part = pl.ds(number * half, half)
        pre = lax.dot_general(rows[...], slab_ref[0], contract, preferred_element_type=jnp.float32)
        hidden_ref[part, :] = (act_ref[part, :] * pre).astype(jnp.bfloat16)


def down_kernel(count, me_ref, *refs):
    pieces, slab_ref = refs[:count], refs[count]
    place(me_ref, pieces, slab_ref)


def slab_call(kernel, name, me, wide, act, pieces, out_type):
    block_rows, width = pieces[0].shape
    model = width * len(pieces)
    tile = row_tile(block_rows)
    rows = sum(value.shape[0] for value in wide)
    in_specs = [pl.BlockSpec(value.shape, lambda t, me: (0, 0)) for value in wide]
    if act is not None:
        in_specs.append(pl.BlockSpec((rows, tile), lambda t, me: (0, t)))
    in_specs += [pl.BlockSpec((tile, width), lambda t, me: (t, 0))] * len(pieces)
    out_specs = [pl.BlockSpec((1, tile, model), lambda t, me: (0, t, 0))]
    out_shape = [jax.ShapeDtypeStruct((1, block_rows, model), jnp.bfloat16)]
    if out_type is not None:
        out_specs.append(pl.BlockSpec((rows, tile), lambda t, me: (0, t)))
        out_shape.append(jax.ShapeDtypeStruct((rows, block_rows), out_type))
    return pl.pallas_call(
        functools.partial(kernel, len(pieces)),
        grid_spec=pltpu.PrefetchScalarGridSpec(
            num_scalar_prefetch=1,
            grid=(block_rows // tile,),
            in_specs=in_specs,
            out_specs=out_specs,
        ),
        out_shape=out_shape,
        compiler_params=pltpu.CompilerParams(vmem_limit_bytes=24 * 2**20),
        cost_estimate=pl.CostEstimate(
            flops=2 * rows * block_rows * model + 10**8,
            bytes_accessed=4 * block_rows * model,
            transcendentals=0,
        ),
        name=name,
    )(me, *wide, *(() if act is None else (act,)), *pieces)


def local(tokens, norm_gain, gate_master, up_master, down_master, routes, route_logits):
    tok_rows = tokens.shape[0]
    block_rows = gate_master.shape[1]
    slabs = lax.axis_size("tp")
    blocks = lax.axis_size("fs")
    experts = slabs // 2
    capacity = tok_rows * routes.shape[1] // experts
    half_cap = capacity // 2
    me = lax.axis_index("tp")
    me_ref = me.astype(jnp.int32)[None]

    def ready(master, mask, scaled):
        piece = lax.dynamic_index_in_dim(master, me ^ mask, 0, keepdims=False)
        if scaled:
            piece = piece * norm_gain[None, :]
        return piece.astype(jnp.bfloat16)

    order = [mask for mask in (6, 7, 2, 4, 3, 5) if mask < slabs]
    order += [mask for mask in range(8, slabs)] + [1, 0]

    def deliver(master, scaled, scope):
        got = {m: swap(ready(master, m, scaled), "tp", m, f"{scope}{m}") for m in order}
        return [got[m] for m in range(slabs)]

    gate_pieces = deliver(gate_master, True, "gate")

    first_prob = jax.nn.sigmoid(route_logits[:, 0] - route_logits[:, 1])
    choice_prob = jnp.stack([first_prob, 1.0 - first_prob], axis=1)
    expert_ids = jnp.arange(experts, dtype=jnp.int32)
    matches = (routes[:, :, None] == expert_ids[None, None, :]).astype(jnp.float32)
    chosen = jnp.sum(matches, axis=1)
    weight = jnp.sum(matches * choice_prob[:, :, None], axis=1)
    position = jnp.cumsum(chosen, axis=0) - 1.0
    slot_ids = jnp.arange(capacity, dtype=jnp.float32)
    placed = chosen.T[:, None, :] * (position.T[:, None, :] == slot_ids[None, :, None]).astype(
        jnp.float32
    )
    placed = placed.astype(jnp.bfloat16)
    picked = jnp.dot(
        placed.reshape(experts * capacity, tok_rows), tokens, preferred_element_type=jnp.float32
    )
    picked = picked.astype(jnp.bfloat16).reshape(slabs, half_cap, tokens.shape[1])
    chunks = [
        swap(lax.dynamic_index_in_dim(picked, me ^ m, 0, keepdims=False), "tp", m, f"tok{m}")
        for m in range(slabs)
    ]
    normed = norm_rows(me_ref, chunks)
    direct = blocks <= 8
    if direct:
        mine = jnp.concatenate([swap(normed, "fs", z, f"row{z}") for z in range(blocks)], axis=0)
    else:
        mine = lax.all_gather(normed, "fs", axis=0, tiled=True)
    theirs = swap(mine, "tp", 1, "rows")

    up_pieces = deliver(up_master, True, "up")
    down_pieces = deliver(down_master, False, "down")

    gate_serve, act = slab_call(
        gate_kernel, "gate_slab", me_ref, (mine, theirs), None, gate_pieces, jnp.float32
    )
    up_serve, hidden = slab_call(
        up_kernel, "up_slab", me_ref, (mine, theirs), act, up_pieces, jnp.bfloat16
    )
    half = blocks * half_cap
    hidden_mine, hidden_theirs = hidden[:half], hidden[half:]

    mixed = jnp.zeros((tok_rows, tokens.shape[1]), jnp.float32)
    for pair in [p for p in (0, 1, 2, 3) if p < experts] + list(range(4, experts)):
        columns = [down_pieces[2 * pair], down_pieces[2 * pair + 1]]
        sent = jnp.concatenate(
            [jnp.dot(hidden_theirs, piece, preferred_element_type=jnp.float32) for piece in columns[::-1]],
            axis=1,
        )
        got = swap(sent, "tp", 1, f"sum{pair}")
        own = jnp.concatenate(
            [jnp.dot(hidden_mine, piece, preferred_element_type=jnp.float32) for piece in columns],
            axis=1,
        )
        part = (own + got).astype(jnp.bfloat16).reshape(blocks, half_cap, -1)
        if direct:
            total = sum(
                swap(part[z], "fs", z, f"part{pair}_{z}").astype(jnp.float32)
                for z in range(blocks)
            )
        else:
            gathered = lax.all_to_all(part, "fs", split_axis=0, concat_axis=0, tiled=True)
            total = jnp.sum(gathered.astype(jnp.float32), axis=0)
        out = total.astype(jnp.bfloat16)
        width = out.shape[1] // 2
        back = [
            swap(out[:, k * width : (k + 1) * width], "tp", 2 * pair + k, f"back{pair}_{k}")
            for k in range(2)
        ]
        expert = (me // 2) ^ pair
        parity = me % 2
        rows = jnp.concatenate(
            [jnp.where(parity == 0, back[0], back[1]), jnp.where(parity == 0, back[1], back[0])]
        )
        one_hot = lax.dynamic_index_in_dim(placed, expert, 0, keepdims=False)
        term = lax.dot_general(
            one_hot, rows, (((0,), (0,)), ((), ())), preferred_element_type=jnp.float32
        )
        mixed = mixed + lax.dynamic_index_in_dim(weight, expert, 1, keepdims=True) * term

    (down_serve,) = slab_call(down_kernel, "down_slab", me_ref, (), None, down_pieces, None)
    return (gate_serve, up_serve, down_serve, mixed.astype(jnp.bfloat16))


def solution(mesh):
    placed = (
        P("fs", "tp"),
        P("tp"),
        P(None, "fs", "tp"),
        P(None, "fs", "tp"),
        P(None, "fs", "tp"),
        P("fs", None),
        P("fs", None),
    )
    return jax.shard_map(
        local,
        mesh=mesh,
        in_specs=placed,
        out_specs=(P("tp", "fs", None), P("tp", "fs", None), P("tp", "fs", None), P("fs", "tp")),
        check_vma=False,
    )
```

```python
import functools

import jax
import jax.numpy as jnp
from jax import lax
from jax.experimental import pallas as pl
from jax.experimental.pallas import tpu as pltpu
from jax.sharding import PartitionSpec as P


epsilon = 1e-05


def swap(value, axis, mask):
    if mask == 0:
        return value
    pairs = [(source, source ^ mask) for source in range(lax.axis_size(axis))]
    return lax.ppermute(value, axis, pairs)


def row_tile(rows):
    return rows // 2 if rows > 256 and rows % 32 == 0 else rows


def norm_kernel(me_ref, *refs):
    chunks, out_ref = refs[:-1], refs[-1]
    width = chunks[0].shape[1]
    total = jnp.zeros((chunks[0].shape[0], 1), jnp.float32)
    for ref in chunks:
        wide = ref[...].astype(jnp.float32)
        total = total + jnp.sum(wide * wide, axis=1, keepdims=True)
    scale = lax.rsqrt(total / (width * len(chunks)) + epsilon)
    for mask, ref in enumerate(chunks):
        start = pl.multiple_of((me_ref[0] ^ mask) * width, width)
        out_ref[:, pl.ds(start, width)] = (ref[...].astype(jnp.float32) * scale).astype(
            jnp.bfloat16
        )


def norm_rows(me, chunks):
    rows, width = chunks[0].shape
    return pl.pallas_call(
        norm_kernel,
        out_shape=jax.ShapeDtypeStruct((rows, width * len(chunks)), jnp.bfloat16),
        in_specs=[pl.BlockSpec(memory_space=pltpu.SMEM)]
        + [pl.BlockSpec(memory_space=pltpu.VMEM)] * len(chunks),
        out_specs=pl.BlockSpec(memory_space=pltpu.VMEM),
        cost_estimate=pl.CostEstimate(flops=10**8, bytes_accessed=10**6, transcendentals=0),
        name="norm_rows",
    )(me, *chunks)


def ready_kernel(masks, me_ref, master_ref, *refs):
    count = len(masks)
    outs, held, arrived = refs[-count - 2 : -2], refs[-2], refs[-1]
    gain = refs[0][...] if len(refs) > count + 2 else None
    copies = [
        pltpu.make_async_copy(master_ref.at[me_ref[0] ^ mask], held.at[k], arrived.at[k])
        for k, mask in enumerate(masks)
    ]
    for copy in copies:
        copy.start()
    for k, copy in enumerate(copies):
        copy.wait()
        piece = held[k] if gain is None else held[k] * gain
        outs[k][...] = piece.astype(jnp.bfloat16)


def ready(master, gain, me, masks):
    _, rows, width = master.shape
    count = len(masks)
    in_specs = [pl.BlockSpec(memory_space=pltpu.SMEM), pl.BlockSpec(memory_space=pltpu.HBM)]
    inputs = [me, master]
    if gain is not None:
        in_specs.append(pl.BlockSpec(memory_space=pltpu.VMEM))
        inputs.append(gain[None, :])
    return pl.pallas_call(
        functools.partial(ready_kernel, masks),
        in_specs=in_specs,
        out_specs=[pl.BlockSpec(memory_space=pltpu.VMEM)] * count,
        out_shape=[jax.ShapeDtypeStruct((rows, width), jnp.bfloat16)] * count,
        scratch_shapes=[
            pltpu.VMEM((count, rows, width), jnp.float32),
            pltpu.SemaphoreType.DMA((count,)),
        ],
        compiler_params=pltpu.CompilerParams(vmem_limit_bytes=60 * 2**20),
        cost_estimate=pl.CostEstimate(
            flops=10**8, bytes_accessed=6 * count * rows * width, transcendentals=0
        ),
    )(*inputs)


contract = (((1,), (1,)), ((), ()))


def place(me_ref, pieces, slab_ref):
    width = pieces[0].shape[1]
    for mask, ref in enumerate(pieces):
        start = pl.multiple_of((me_ref[0] ^ mask) * width, width)
        slab_ref[0, :, pl.ds(start, width)] = ref[...]


def gate_kernel(count, me_ref, mine_ref, theirs_ref, *refs):
    pieces, (slab_ref, act_ref) = refs[:count], refs[count:]
    place(me_ref, pieces, slab_ref)
    half = mine_ref.shape[0]
    for number, rows in enumerate((mine_ref, theirs_ref)):
        pre = lax.dot_general(rows[...], slab_ref[0], contract, preferred_element_type=jnp.float32)
        act_ref[0, pl.ds(number * half, half), :] = pre * (1.0 / (1.0 + jnp.exp(-pre)))


def up_kernel(count, me_ref, mine_ref, theirs_ref, act_ref, *refs):
    pieces, (slab_ref, hidden_ref) = refs[:count], refs[count:]
    place(me_ref, pieces, slab_ref)
    half = mine_ref.shape[0]
    for number, rows in enumerate((mine_ref, theirs_ref)):
        part = pl.ds(number * half, half)
        pre = lax.dot_general(rows[...], slab_ref[0], contract, preferred_element_type=jnp.float32)
        hidden_ref[0, part, :] = (act_ref[0, part, :] * pre).astype(jnp.bfloat16)


def fill_kernel(masks, me_ref, *refs):
    count = len(masks)
    pieces, slab_ref, left = refs[:count], refs[-2], refs[-1]
    width = pieces[0].shape[1]
    copies = []
    for k, mask in enumerate(masks):
        start = pl.multiple_of((me_ref[0] ^ mask) * width, width)
        copies.append(
            pltpu.make_async_copy(pieces[k], slab_ref.at[0, :, pl.ds(start, width)], left.at[k])
        )
    for copy in copies:
        copy.start()
    for copy in copies:
        copy.wait()


def fill_call(me, pieces, masks, model, slab):
    rows, width = pieces[0].shape
    count = len(masks)
    in_specs = [pl.BlockSpec(memory_space=pltpu.SMEM)]
    in_specs += [pl.BlockSpec(memory_space=pltpu.VMEM)] * count
    inputs = [me, *pieces]
    if slab is not None:
        in_specs.append(pl.BlockSpec(memory_space=pl.ANY))
        inputs.append(slab)
    return pl.pallas_call(
        functools.partial(fill_kernel, masks),
        in_specs=in_specs,
        out_specs=pl.BlockSpec(memory_space=pl.ANY),
        out_shape=jax.ShapeDtypeStruct((1, rows, model), jnp.bfloat16),
        input_output_aliases={} if slab is None else {1 + count: 0},
        scratch_shapes=[pltpu.SemaphoreType.DMA((count,))],
        compiler_params=pltpu.CompilerParams(vmem_limit_bytes=52 * 2**20),
        cost_estimate=pl.CostEstimate(
            flops=10**8, bytes_accessed=4 * count * rows * width, transcendentals=0
        ),
    )(*inputs)


def slab_call(kernel, me, wide, act, pieces, out_type):
    block_rows, width = pieces[0].shape
    model = width * len(pieces)
    tile = row_tile(block_rows)
    rows = sum(value.shape[0] for value in wide)
    in_specs = [pl.BlockSpec(value.shape, lambda t, me: (0, 0)) for value in wide]
    if act is not None:
        in_specs.append(pl.BlockSpec((1, rows, tile), lambda t, me: (t, 0, 0)))
    in_specs += [pl.BlockSpec((tile, width), lambda t, me: (t, 0))] * len(pieces)
    out_specs = [pl.BlockSpec((1, tile, model), lambda t, me: (0, t, 0))]
    out_shape = [jax.ShapeDtypeStruct((1, block_rows, model), jnp.bfloat16)]
    if out_type is not None:
        out_specs.append(pl.BlockSpec((1, rows, tile), lambda t, me: (t, 0, 0)))
        out_shape.append(jax.ShapeDtypeStruct((block_rows // tile, rows, tile), out_type))
    return pl.pallas_call(
        functools.partial(kernel, len(pieces)),
        grid_spec=pltpu.PrefetchScalarGridSpec(
            num_scalar_prefetch=1,
            grid=(block_rows // tile,),
            in_specs=in_specs,
            out_specs=out_specs,
        ),
        out_shape=out_shape,
        compiler_params=pltpu.CompilerParams(vmem_limit_bytes=52 * 2**20),
        cost_estimate=pl.CostEstimate(
            flops=2 * rows * block_rows * model + 10**8,
            bytes_accessed=4 * block_rows * model,
            transcendentals=0,
        ),
    )(me, *wide, *(() if act is None else (act,)), *pieces)


def dots_kernel(count, hidden_ref, *refs):
    pieces, (sent_ref, own_ref) = refs[:count], refs[count:]
    blocks, _, rows, width = own_ref.shape
    half = blocks * rows
    tiles, _, tile = hidden_ref.shape
    for number, ref in enumerate(pieces):
        for target, slot, start in ((sent_ref, number ^ 1, half), (own_ref, number, 0)):
            out = sum(
                jnp.dot(
                    hidden_ref[t, start : start + half],
                    ref[t * tile : (t + 1) * tile],
                    preferred_element_type=jnp.float32,
                )
                for t in range(tiles)
            )
            target[:, slot] = out.reshape(blocks, rows, width)


def dots_call(hidden, pieces, blocks):
    rows = hidden.shape[1]
    inner, width = pieces[0].shape
    out = jax.ShapeDtypeStruct((blocks, len(pieces), rows // 2 // blocks, width), jnp.float32)
    return pl.pallas_call(
        functools.partial(dots_kernel, len(pieces)),
        in_specs=[pl.BlockSpec(memory_space=pltpu.VMEM)] * (1 + len(pieces)),
        out_specs=[pl.BlockSpec(memory_space=pltpu.VMEM)] * 2,
        out_shape=[out, out],
        compiler_params=pltpu.CompilerParams(vmem_limit_bytes=52 * 2**20),
        cost_estimate=pl.CostEstimate(
            flops=2 * rows * inner * width * len(pieces) + 10**8,
            bytes_accessed=2 * inner * width * len(pieces),
            transcendentals=0,
        ),
    )(hidden, *pieces)


def local(tokens, norm_gain, gate_master, up_master, down_master, routes, route_logits):
    tok_rows = tokens.shape[0]
    slabs = lax.axis_size("tp")
    blocks = lax.axis_size("fs")
    experts = slabs // 2
    capacity = tok_rows * routes.shape[1] // experts
    half_cap = capacity // 2
    me = lax.axis_index("tp")
    me_ref = me.astype(jnp.int32)[None]

    def deliver(master, gain, groups):
        got = {}
        for masks in groups:
            pieces = ready(master, gain, me_ref, masks)
            for mask, piece in zip(masks, pieces):
                got[mask] = swap(piece, "tp", mask)
        return [got[mask] for mask in range(slabs)]

    first_groups, groups = piece_groups(slabs)
    gate_pieces = deliver(gate_master, norm_gain, first_groups)

    first_prob = jax.nn.sigmoid(route_logits[:, 0] - route_logits[:, 1])
    choice_prob = jnp.stack([first_prob, 1.0 - first_prob], axis=1)
    expert_ids = jnp.arange(experts, dtype=jnp.int32)
    matches = (routes[:, :, None] == expert_ids[None, None, :]).astype(jnp.float32)
    chosen = jnp.sum(matches, axis=1)
    weight = jnp.sum(matches * choice_prob[:, :, None], axis=1)
    position = jnp.cumsum(chosen, axis=0) - 1.0
    slot_ids = jnp.arange(capacity, dtype=jnp.float32)
    placed = chosen.T[:, None, :] * (position.T[:, None, :] == slot_ids[None, :, None]).astype(
        jnp.float32
    )
    placed = placed.astype(jnp.bfloat16)
    by_slab = placed.reshape(slabs, half_cap, tok_rows)
    spread = [
        jnp.concatenate([lax.dynamic_index_in_dim(by_slab, me ^ m, 0, False) for m in (2 * p, 2 * p + 1)])
        for p in range(experts)
    ]
    share = [lax.dynamic_index_in_dim(weight, (me // 2) ^ p, 1) for p in range(experts)]
    picked = jnp.dot(
        placed.reshape(experts * capacity, tok_rows), tokens, preferred_element_type=jnp.float32
    )
    picked = picked.astype(jnp.bfloat16).reshape(slabs, half_cap, tokens.shape[1])
    chunks = [
        swap(lax.dynamic_index_in_dim(picked, me ^ m, 0, keepdims=False), "tp", m)
        for m in range(slabs)
    ]
    normed = norm_rows(me_ref, chunks)
    direct = blocks <= 8
    if direct:
        gathered = [swap(normed, "fs", z) for z in range(blocks)]
        mine = jnp.concatenate(gathered, axis=0)
    else:
        mine = lax.all_gather(normed, "fs", axis=0, tiled=True)
    theirs = swap(mine, "tp", 1)

    up_pieces = deliver(up_master, norm_gain, groups)
    down_pieces = deliver(down_master, None, groups)

    gate_serve, act = slab_call(gate_kernel, me_ref, (mine, theirs), None, gate_pieces, jnp.float32)
    up_serve, hidden = slab_call(up_kernel, me_ref, (mine, theirs), act, up_pieces, jnp.bfloat16)
    backs = {}
    down_serve = None
    pairs = pair_groups(experts)
    for number, group in enumerate(pairs):
        masks = [mask for pair in group for mask in (2 * pair, 2 * pair + 1)]
        sent, own = dots_call(hidden, [down_pieces[m] for m in masks], blocks)
        got = swap(sent, "tp", 1)
        parts = [(own[z] + got[z]).astype(jnp.bfloat16) for z in range(blocks)]
        if direct:
            parts = [swap(part, "fs", z) for z, part in enumerate(parts)]
        else:
            parts = lax.all_to_all(jnp.stack(parts), "fs", split_axis=0, concat_axis=0, tiled=True)
        for k, mask in enumerate(masks):
            total = sum(parts[z][k].astype(jnp.float32) for z in range(blocks))
            total = total.astype(jnp.bfloat16)
            backs[mask] = swap(total, "tp", mask)
        if number > 0:
            filled = masks if number > 1 else [0, 1] + masks
            pieces = [down_pieces[m] for m in filled]
            model = down_pieces[0].shape[1] * slabs
            down_serve = fill_call(me_ref, pieces, filled, model, down_serve)

    mixed = jnp.zeros((tok_rows, tokens.shape[1]), jnp.float32)
    for pair in range(experts):
        rows = jnp.concatenate([backs[2 * pair], backs[2 * pair + 1]])
        term = lax.dot_general(
            spread[pair], rows, (((0,), (0,)), ((), ())), preferred_element_type=jnp.float32
        )
        mixed = mixed + share[pair] * term

    return (gate_serve, up_serve, down_serve, mixed.astype(jnp.bfloat16))


def piece_groups(slabs):
    order = [mask for mask in (4, 2, 5, 3, 6, 7, *range(8, slabs)) if mask < slabs] + [1, 0]
    return [order[:2], order[2:]], [order]


def pair_groups(experts):
    return [[0], [*range(1, experts - 1)], [experts - 1]]


def solution(mesh):
    placed = (
        P("fs", "tp"),
        P("tp"),
        P(None, "fs", "tp"),
        P(None, "fs", "tp"),
        P(None, "fs", "tp"),
        P("fs", None),
        P("fs", None),
    )
    return jax.shard_map(
        local,
        mesh=mesh,
        in_specs=placed,
        out_specs=(P("tp", "fs", None), P("tp", "fs", None), P("tp", "fs", None), P("fs", "tp")),
        check_vma=False,
    )
```

```python
import functools

import jax
import jax.numpy as jnp
from jax import lax
from jax.experimental import pallas as pl
from jax.experimental.pallas import tpu as pltpu
from jax.sharding import PartitionSpec as P


epsilon = 1e-05


def swap(value, axis, mask):
    if mask == 0:
        return value
    pairs = [(source, source ^ mask) for source in range(lax.axis_size(axis))]
    return lax.ppermute(value, axis, pairs)


def row_tile(rows):
    return rows // 2 if rows > 256 and rows % 32 == 0 else rows


def norm_kernel(me_ref, *refs):
    chunks, out_ref = refs[:-1], refs[-1]
    width = chunks[0].shape[1]
    total = jnp.zeros((chunks[0].shape[0], 1), jnp.float32)
    for ref in chunks:
        wide = ref[...].astype(jnp.float32)
        total = total + jnp.sum(wide * wide, axis=1, keepdims=True)
    scale = lax.rsqrt(total / (width * len(chunks)) + epsilon)
    for mask, ref in enumerate(chunks):
        start = pl.multiple_of((me_ref[0] ^ mask) * width, width)
        out_ref[:, pl.ds(start, width)] = (ref[...].astype(jnp.float32) * scale).astype(
            jnp.bfloat16
        )


def norm_rows(me, chunks):
    rows, width = chunks[0].shape
    return pl.pallas_call(
        norm_kernel,
        out_shape=jax.ShapeDtypeStruct((rows, width * len(chunks)), jnp.bfloat16),
        in_specs=[pl.BlockSpec(memory_space=pltpu.SMEM)]
        + [pl.BlockSpec(memory_space=pltpu.VMEM)] * len(chunks),
        out_specs=pl.BlockSpec(memory_space=pltpu.VMEM),
        cost_estimate=pl.CostEstimate(flops=10**8, bytes_accessed=10**6, transcendentals=0),
        name="norm_rows",
    )(me, *chunks)


def ready_kernel(masks, me_ref, master_ref, *refs):
    count = len(masks)
    outs, held, arrived = refs[-count - 2 : -2], refs[-2], refs[-1]
    gain = refs[0][...] if len(refs) > count + 2 else None
    copies = [
        pltpu.make_async_copy(master_ref.at[me_ref[0] ^ mask], held.at[k], arrived.at[k])
        for k, mask in enumerate(masks)
    ]
    for copy in copies:
        copy.start()
    for k, copy in enumerate(copies):
        copy.wait()
        piece = held[k] if gain is None else held[k] * gain
        outs[k][...] = piece.astype(jnp.bfloat16)


def ready(master, gain, me, masks):
    _, rows, width = master.shape
    count = len(masks)
    in_specs = [pl.BlockSpec(memory_space=pltpu.SMEM), pl.BlockSpec(memory_space=pltpu.HBM)]
    inputs = [me, master]
    if gain is not None:
        in_specs.append(pl.BlockSpec(memory_space=pltpu.VMEM))
        inputs.append(gain[None, :])
    return pl.pallas_call(
        functools.partial(ready_kernel, masks),
        in_specs=in_specs,
        out_specs=[pl.BlockSpec(memory_space=pltpu.VMEM)] * count,
        out_shape=[jax.ShapeDtypeStruct((rows, width), jnp.bfloat16)] * count,
        scratch_shapes=[
            pltpu.VMEM((count, rows, width), jnp.float32),
            pltpu.SemaphoreType.DMA((count,)),
        ],
        compiler_params=pltpu.CompilerParams(vmem_limit_bytes=57 * 2**20),
        cost_estimate=pl.CostEstimate(
            flops=10**8, bytes_accessed=6 * count * rows * width, transcendentals=0
        ),
    )(*inputs)


contract = (((1,), (1,)), ((), ()))


def place(me_ref, pieces, slab_ref):
    width = pieces[0].shape[1]
    for mask, ref in enumerate(pieces):
        start = pl.multiple_of((me_ref[0] ^ mask) * width, width)
        slab_ref[0, :, pl.ds(start, width)] = ref[...]


def gate_kernel(count, me_ref, mine_ref, theirs_ref, *refs):
    pieces, (slab_ref, act_ref) = refs[:count], refs[count:]
    place(me_ref, pieces, slab_ref)
    half = mine_ref.shape[0]
    for number, rows in enumerate((mine_ref, theirs_ref)):
        pre = lax.dot_general(rows[...], slab_ref[0], contract, preferred_element_type=jnp.float32)
        act_ref[0, pl.ds(number * half, half), :] = pre * (1.0 / (1.0 + jnp.exp(-pre)))


def up_kernel(count, me_ref, mine_ref, theirs_ref, act_ref, *refs):
    pieces, (slab_ref, hidden_ref) = refs[:count], refs[count:]
    place(me_ref, pieces, slab_ref)
    half = mine_ref.shape[0]
    for number, rows in enumerate((mine_ref, theirs_ref)):
        part = pl.ds(number * half, half)
        pre = lax.dot_general(rows[...], slab_ref[0], contract, preferred_element_type=jnp.float32)
        hidden_ref[0, part, :] = (act_ref[0, part, :] * pre).astype(jnp.bfloat16)


def fill_kernel(masks, me_ref, *refs):
    count = len(masks)
    pieces, slab_ref, left = refs[:count], refs[-2], refs[-1]
    width = pieces[0].shape[1]
    copies = []
    for k, mask in enumerate(masks):
        start = pl.multiple_of((me_ref[0] ^ mask) * width, width)
        copies.append(
            pltpu.make_async_copy(pieces[k], slab_ref.at[0, :, pl.ds(start, width)], left.at[k])
        )
    for copy in copies:
        copy.start()
    for copy in copies:
        copy.wait()


def fill_call(me, pieces, masks, model, slab):
    rows, width = pieces[0].shape
    count = len(masks)
    in_specs = [pl.BlockSpec(memory_space=pltpu.SMEM)]
    in_specs += [pl.BlockSpec(memory_space=pltpu.VMEM)] * count
    inputs = [me, *pieces]
    if slab is not None:
        in_specs.append(pl.BlockSpec(memory_space=pl.ANY))
        inputs.append(slab)
    return pl.pallas_call(
        functools.partial(fill_kernel, masks),
        in_specs=in_specs,
        out_specs=pl.BlockSpec(memory_space=pl.ANY),
        out_shape=jax.ShapeDtypeStruct((1, rows, model), jnp.bfloat16),
        input_output_aliases={} if slab is None else {1 + count: 0},
        scratch_shapes=[pltpu.SemaphoreType.DMA((count,))],
        compiler_params=pltpu.CompilerParams(vmem_limit_bytes=16 * 2**20),
        cost_estimate=pl.CostEstimate(
            flops=10**8, bytes_accessed=4 * count * rows * width, transcendentals=0
        ),
    )(*inputs)


def slab_call(kernel, me, wide, act, pieces, out_type):
    block_rows, width = pieces[0].shape
    model = width * len(pieces)
    tile = row_tile(block_rows)
    rows = sum(value.shape[0] for value in wide)
    in_specs = [pl.BlockSpec(value.shape, lambda t, me: (0, 0)) for value in wide]
    if act is not None:
        in_specs.append(pl.BlockSpec((1, rows, tile), lambda t, me: (t, 0, 0)))
    in_specs += [pl.BlockSpec((tile, width), lambda t, me: (t, 0))] * len(pieces)
    out_specs = [pl.BlockSpec((1, tile, model), lambda t, me: (0, t, 0))]
    out_shape = [jax.ShapeDtypeStruct((1, block_rows, model), jnp.bfloat16)]
    if out_type is not None:
        out_specs.append(pl.BlockSpec((1, rows, tile), lambda t, me: (t, 0, 0)))
        out_shape.append(jax.ShapeDtypeStruct((block_rows // tile, rows, tile), out_type))
    return pl.pallas_call(
        functools.partial(kernel, len(pieces)),
        grid_spec=pltpu.PrefetchScalarGridSpec(
            num_scalar_prefetch=1,
            grid=(block_rows // tile,),
            in_specs=in_specs,
            out_specs=out_specs,
        ),
        out_shape=out_shape,
        compiler_params=pltpu.CompilerParams(vmem_limit_bytes=24 * 2**20),
        cost_estimate=pl.CostEstimate(
            flops=2 * rows * block_rows * model + 10**8,
            bytes_accessed=4 * block_rows * model,
            transcendentals=0,
        ),
    )(me, *wide, *(() if act is None else (act,)), *pieces)


def dots_kernel(count, hidden_ref, *refs):
    pieces, (sent_ref, own_ref) = refs[:count], refs[count:]
    blocks, _, rows, width = own_ref.shape
    half = blocks * rows
    tiles, _, tile = hidden_ref.shape
    for number, ref in enumerate(pieces):
        for target, slot, start in ((sent_ref, number ^ 1, half), (own_ref, number, 0)):
            out = sum(
                jnp.dot(
                    hidden_ref[t, start : start + half],
                    ref[t * tile : (t + 1) * tile],
                    preferred_element_type=jnp.float32,
                )
                for t in range(tiles)
            )
            target[:, slot] = out.reshape(blocks, rows, width).astype(target.dtype)


def dots_call(hidden, pieces, blocks):
    rows = hidden.shape[1]
    inner, width = pieces[0].shape
    shape = (blocks, len(pieces), rows // 2 // blocks, width)
    outs = [jax.ShapeDtypeStruct(shape, kind) for kind in (jnp.bfloat16, jnp.float32)]
    return pl.pallas_call(
        functools.partial(dots_kernel, len(pieces)),
        in_specs=[pl.BlockSpec(memory_space=pltpu.VMEM)] * (1 + len(pieces)),
        out_specs=[pl.BlockSpec(memory_space=pltpu.VMEM)] * 2,
        out_shape=outs,
        compiler_params=pltpu.CompilerParams(vmem_limit_bytes=16 * 2**20),
        cost_estimate=pl.CostEstimate(
            flops=2 * rows * inner * width * len(pieces) + 10**8,
            bytes_accessed=2 * inner * width * len(pieces),
            transcendentals=0,
        ),
    )(hidden, *pieces)


def local(tokens, norm_gain, gate_master, up_master, down_master, routes, route_logits):
    tok_rows = tokens.shape[0]
    slabs = lax.axis_size("tp")
    blocks = lax.axis_size("fs")
    experts = slabs // 2
    capacity = tok_rows * routes.shape[1] // experts
    half_cap = capacity // 2
    me = lax.axis_index("tp")
    me_ref = me.astype(jnp.int32)[None]

    def deliver(master, gain, groups):
        got = {}
        for masks in groups:
            pieces = ready(master, gain, me_ref, masks)
            for mask, piece in zip(masks, pieces):
                got[mask] = swap(piece, "tp", mask)
        return [got[mask] for mask in range(slabs)]

    first_groups, groups = piece_groups(slabs)
    gate_pieces = deliver(gate_master, norm_gain, first_groups)

    first_prob = jax.nn.sigmoid(route_logits[:, 0] - route_logits[:, 1])
    choice_prob = jnp.stack([first_prob, 1.0 - first_prob], axis=1)
    expert_ids = jnp.arange(experts, dtype=jnp.int32)
    matches = (routes[:, :, None] == expert_ids[None, None, :]).astype(jnp.float32)
    chosen = jnp.sum(matches, axis=1)
    weight = jnp.sum(matches * choice_prob[:, :, None], axis=1)
    position = jnp.cumsum(chosen, axis=0) - 1.0
    slot_ids = jnp.arange(capacity, dtype=jnp.float32)
    placed = chosen.T[:, None, :] * (position.T[:, None, :] == slot_ids[None, :, None]).astype(
        jnp.float32
    )
    placed = placed.astype(jnp.bfloat16)
    by_slab = placed.reshape(slabs, half_cap, tok_rows)
    spread = [
        jnp.concatenate([lax.dynamic_index_in_dim(by_slab, me ^ m, 0, False) for m in (2 * p, 2 * p + 1)])
        for p in range(experts)
    ]
    share = [lax.dynamic_index_in_dim(weight, (me // 2) ^ p, 1) for p in range(experts)]
    picked = jnp.dot(
        placed.reshape(experts * capacity, tok_rows), tokens, preferred_element_type=jnp.float32
    )
    picked = picked.astype(jnp.bfloat16).reshape(slabs, half_cap, tokens.shape[1])
    picked, spread, share = lax.optimization_barrier((picked, spread, share))
    chunks = [
        swap(lax.dynamic_index_in_dim(picked, me ^ m, 0, keepdims=False), "tp", m)
        for m in range(slabs)
    ]
    normed = norm_rows(me_ref, chunks)
    direct = blocks <= 8
    if direct:
        gathered = [swap(normed, "fs", z) for z in range(blocks)]
        mine = jnp.concatenate(gathered, axis=0)
    else:
        mine = lax.all_gather(normed, "fs", axis=0, tiled=True)
    theirs = swap(mine, "tp", 1)

    up_pieces = deliver(up_master, norm_gain, groups)
    down_pieces = deliver(down_master, None, groups)

    gate_serve, act = slab_call(gate_kernel, me_ref, (mine, theirs), None, gate_pieces, jnp.float32)
    up_serve, hidden = slab_call(up_kernel, me_ref, (mine, theirs), act, up_pieces, jnp.bfloat16)
    backs = {}
    down_serve = None
    pairs = pair_groups(experts)
    for number, group in enumerate(pairs):
        masks = [mask for pair in group for mask in (2 * pair, 2 * pair + 1)]
        sent, own = dots_call(hidden, [down_pieces[m] for m in masks], blocks)
        got = swap(sent, "tp", 1)
        parts = [(own[z] + got[z].astype(jnp.float32)).astype(jnp.bfloat16) for z in range(blocks)]
        if direct:
            parts = [swap(part, "fs", z) for z, part in enumerate(parts)]
        else:
            parts = lax.all_to_all(jnp.stack(parts), "fs", split_axis=0, concat_axis=0, tiled=True)
        for k, mask in enumerate(masks):
            total = sum(parts[z][k].astype(jnp.float32) for z in range(blocks))
            total = total.astype(jnp.bfloat16)
            backs[mask] = swap(total, "tp", mask)
        if number > 0:
            filled = masks if number > 1 else [0, 1] + masks
            pieces = [down_pieces[m] for m in filled]
            model = down_pieces[0].shape[1] * slabs
            down_serve = fill_call(me_ref, pieces, filled, model, down_serve)

    mixed = jnp.zeros((tok_rows, tokens.shape[1]), jnp.float32)
    for pair in reversed(range(experts)):
        rows = jnp.concatenate([backs[2 * pair], backs[2 * pair + 1]])
        term = lax.dot_general(
            spread[pair], rows, (((0,), (0,)), ((), ())), preferred_element_type=jnp.float32
        )
        mixed = mixed + share[pair] * term

    return (gate_serve, up_serve, down_serve, mixed.astype(jnp.bfloat16))


def piece_groups(slabs):
    order = [mask for mask in (4, 2, 5, 3, 6, 7, *range(8, slabs)) if mask < slabs] + [1, 0]
    return [order[:2], order[2:]], [order]


def pair_groups(experts):
    return [[0], [*range(1, experts - 1)], [experts - 1]]


def solution(mesh):
    placed = (
        P("fs", "tp"),
        P("tp"),
        P(None, "fs", "tp"),
        P(None, "fs", "tp"),
        P(None, "fs", "tp"),
        P("fs", None),
        P("fs", None),
    )
    return jax.shard_map(
        local,
        mesh=mesh,
        in_specs=placed,
        out_specs=(P("tp", "fs", None), P("tp", "fs", None), P("tp", "fs", None), P("fs", "tp")),
        check_vma=False,
    )
```

```python
import functools

import jax
import jax.numpy as jnp
from jax import lax
from jax.experimental import pallas as pl
from jax.experimental.pallas import tpu as pltpu
from jax.sharding import PartitionSpec as P


epsilon = 1e-05


def swap(value, axis, mask):
    if mask == 0:
        return value
    pairs = [(source, source ^ mask) for source in range(lax.axis_size(axis))]
    return lax.ppermute(value, axis, pairs)


def row_tile(rows):
    return rows // 2 if rows > 256 and rows % 32 == 0 else rows


def norm_kernel(me_ref, *refs):
    chunks, out_ref = refs[:-1], refs[-1]
    width = chunks[0].shape[1]
    total = jnp.zeros((chunks[0].shape[0], 1), jnp.float32)
    for ref in chunks:
        wide = ref[...].astype(jnp.float32)
        total = total + jnp.sum(wide * wide, axis=1, keepdims=True)
    scale = lax.rsqrt(total / (width * len(chunks)) + epsilon)
    for mask, ref in enumerate(chunks):
        start = pl.multiple_of((me_ref[0] ^ mask) * width, width)
        out_ref[:, pl.ds(start, width)] = (ref[...].astype(jnp.float32) * scale).astype(
            jnp.bfloat16
        )


def norm_rows(me, chunks):
    rows, width = chunks[0].shape
    return pl.pallas_call(
        norm_kernel,
        out_shape=jax.ShapeDtypeStruct((rows, width * len(chunks)), jnp.bfloat16),
        in_specs=[pl.BlockSpec(memory_space=pltpu.SMEM)]
        + [pl.BlockSpec(memory_space=pltpu.VMEM)] * len(chunks),
        out_specs=pl.BlockSpec(memory_space=pltpu.VMEM),
        cost_estimate=pl.CostEstimate(flops=10**8, bytes_accessed=10**6, transcendentals=0),
        name="norm_rows",
    )(me, *chunks)


def ready_kernel(masks, me_ref, master_ref, *refs):
    count = len(masks)
    outs, held, arrived = refs[-count - 2 : -2], refs[-2], refs[-1]
    gain = refs[0][...] if len(refs) > count + 2 else None
    copies = [
        pltpu.make_async_copy(master_ref.at[me_ref[0] ^ mask], held.at[k], arrived.at[k])
        for k, mask in enumerate(masks)
    ]
    for copy in copies:
        copy.start()
    for k, copy in enumerate(copies):
        copy.wait()
        piece = held[k] if gain is None else held[k] * gain
        outs[k][...] = piece.astype(jnp.bfloat16)


def ready(master, gain, me, masks):
    _, rows, width = master.shape
    count = len(masks)
    in_specs = [pl.BlockSpec(memory_space=pltpu.SMEM), pl.BlockSpec(memory_space=pltpu.HBM)]
    inputs = [me, master]
    if gain is not None:
        in_specs.append(pl.BlockSpec(memory_space=pltpu.VMEM))
        inputs.append(gain[None, :])
    return pl.pallas_call(
        functools.partial(ready_kernel, masks),
        in_specs=in_specs,
        out_specs=[pl.BlockSpec(memory_space=pltpu.VMEM)] * count,
        out_shape=[jax.ShapeDtypeStruct((rows, width), jnp.bfloat16)] * count,
        scratch_shapes=[
            pltpu.VMEM((count, rows, width), jnp.float32),
            pltpu.SemaphoreType.DMA((count,)),
        ],
        compiler_params=pltpu.CompilerParams(vmem_limit_bytes=57 * 2**20),
        cost_estimate=pl.CostEstimate(
            flops=10**8, bytes_accessed=6 * count * rows * width, transcendentals=0
        ),
    )(*inputs)


contract = (((1,), (1,)), ((), ()))


def place(me_ref, pieces, slab_ref):
    width = pieces[0].shape[1]
    for mask, ref in enumerate(pieces):
        start = pl.multiple_of((me_ref[0] ^ mask) * width, width)
        slab_ref[0, :, pl.ds(start, width)] = ref[...]


def gate_kernel(count, me_ref, mine_ref, theirs_ref, *refs):
    pieces, (slab_ref, act_ref) = refs[:count], refs[count:]
    place(me_ref, pieces, slab_ref)
    half = mine_ref.shape[0]
    for number, rows in enumerate((mine_ref, theirs_ref)):
        pre = lax.dot_general(rows[...], slab_ref[0], contract, preferred_element_type=jnp.float32)
        act_ref[0, pl.ds(number * half, half), :] = pre * (1.0 / (1.0 + jnp.exp(-pre)))


def up_kernel(count, me_ref, mine_ref, theirs_ref, act_ref, *refs):
    pieces, (slab_ref, hidden_ref) = refs[:count], refs[count:]
    place(me_ref, pieces, slab_ref)
    half = mine_ref.shape[0]
    for number, rows in enumerate((mine_ref, theirs_ref)):
        part = pl.ds(number * half, half)
        pre = lax.dot_general(rows[...], slab_ref[0], contract, preferred_element_type=jnp.float32)
        hidden_ref[0, part, :] = (act_ref[0, part, :] * pre).astype(jnp.bfloat16)


def fill_kernel(masks, me_ref, *refs):
    count = len(masks)
    pieces, slab_ref, left = refs[:count], refs[-2], refs[-1]
    width = pieces[0].shape[1]
    copies = []
    for k, mask in enumerate(masks):
        start = pl.multiple_of((me_ref[0] ^ mask) * width, width)
        copies.append(
            pltpu.make_async_copy(pieces[k], slab_ref.at[0, :, pl.ds(start, width)], left.at[k])
        )
    for copy in copies:
        copy.start()
    for copy in copies:
        copy.wait()


def fill_call(me, pieces, masks, model, slab):
    rows, width = pieces[0].shape
    count = len(masks)
    in_specs = [pl.BlockSpec(memory_space=pltpu.SMEM)]
    in_specs += [pl.BlockSpec(memory_space=pltpu.VMEM)] * count
    inputs = [me, *pieces]
    if slab is not None:
        in_specs.append(pl.BlockSpec(memory_space=pl.ANY))
        inputs.append(slab)
    return pl.pallas_call(
        functools.partial(fill_kernel, masks),
        in_specs=in_specs,
        out_specs=pl.BlockSpec(memory_space=pl.ANY),
        out_shape=jax.ShapeDtypeStruct((1, rows, model), jnp.bfloat16),
        input_output_aliases={} if slab is None else {1 + count: 0},
        scratch_shapes=[pltpu.SemaphoreType.DMA((count,))],
        compiler_params=pltpu.CompilerParams(vmem_limit_bytes=16 * 2**20),
        cost_estimate=pl.CostEstimate(
            flops=10**8, bytes_accessed=4 * count * rows * width, transcendentals=0
        ),
    )(*inputs)


def slab_call(kernel, me, wide, act, pieces, out_type):
    block_rows, width = pieces[0].shape
    model = width * len(pieces)
    tile = row_tile(block_rows)
    rows = sum(value.shape[0] for value in wide)
    in_specs = [pl.BlockSpec(value.shape, lambda t, me: (0, 0)) for value in wide]
    if act is not None:
        in_specs.append(pl.BlockSpec((1, rows, tile), lambda t, me: (t, 0, 0)))
    in_specs += [pl.BlockSpec((tile, width), lambda t, me: (t, 0))] * len(pieces)
    out_specs = [pl.BlockSpec((1, tile, model), lambda t, me: (0, t, 0))]
    out_shape = [jax.ShapeDtypeStruct((1, block_rows, model), jnp.bfloat16)]
    if out_type is not None:
        out_specs.append(pl.BlockSpec((1, rows, tile), lambda t, me: (t, 0, 0)))
        out_shape.append(jax.ShapeDtypeStruct((block_rows // tile, rows, tile), out_type))
    return pl.pallas_call(
        functools.partial(kernel, len(pieces)),
        grid_spec=pltpu.PrefetchScalarGridSpec(
            num_scalar_prefetch=1,
            grid=(block_rows // tile,),
            in_specs=in_specs,
            out_specs=out_specs,
        ),
        out_shape=out_shape,
        compiler_params=pltpu.CompilerParams(vmem_limit_bytes=24 * 2**20),
        cost_estimate=pl.CostEstimate(
            flops=2 * rows * block_rows * model + 10**8,
            bytes_accessed=4 * block_rows * model,
            transcendentals=0,
        ),
    )(me, *wide, *(() if act is None else (act,)), *pieces)


def dots_kernel(blocks, own_ref, other_ref, *refs):
    outs = refs[-blocks:]
    count = (len(refs) - blocks) // 2
    tiles, rows, tile = own_ref.shape
    half = rows // 2
    for number in range(count):
        own_piece, other_piece = refs[number], refs[count + number]
        for side in range(2):
            here, there = side * half, (1 - side) * half
            total = sum(
                jnp.dot(
                    hidden[t, start : start + half],
                    piece[t * tile : (t + 1) * tile],
                    preferred_element_type=jnp.float32,
                )
                for hidden, start, piece in ((own_ref, here, own_piece), (other_ref, there, other_piece))
                for t in range(tiles)
            )
            total = total.astype(jnp.bfloat16).reshape(blocks, half // blocks, -1)
            size = half // blocks
            for z in range(blocks):
                outs[z][number, side * size : (side + 1) * size] = total[z]


def dots_call(own, other, own_pieces, other_pieces, blocks):
    rows = own.shape[1]
    inner, width = own_pieces[0].shape
    count = len(own_pieces)
    out = jax.ShapeDtypeStruct((count, rows // blocks, width), jnp.bfloat16)
    return pl.pallas_call(
        functools.partial(dots_kernel, blocks),
        in_specs=[pl.BlockSpec(memory_space=pltpu.VMEM)] * (2 + 2 * count),
        out_specs=[pl.BlockSpec(memory_space=pltpu.VMEM)] * blocks,
        out_shape=[out] * blocks,
        compiler_params=pltpu.CompilerParams(vmem_limit_bytes=16 * 2**20),
        cost_estimate=pl.CostEstimate(
            flops=4 * rows * inner * width * count + 10**8,
            bytes_accessed=4 * inner * width * count,
            transcendentals=0,
        ),
    )(own, other, *own_pieces, *other_pieces)


def local(tokens, norm_gain, gate_master, up_master, down_master, routes, route_logits):
    tok_rows = tokens.shape[0]
    slabs = lax.axis_size("tp")
    blocks = lax.axis_size("fs")
    experts = slabs // 2
    capacity = tok_rows * routes.shape[1] // experts
    half_cap = capacity // 2
    me = lax.axis_index("tp")
    me_ref = me.astype(jnp.int32)[None]

    def deliver(master, gain, groups):
        got = {}
        for masks in groups:
            if len(masks) > 2:
                pieces = ready(master, gain, me_ref, masks)
            else:
                pieces = []
                for mask in masks:
                    piece = lax.dynamic_index_in_dim(master, me ^ mask, 0, keepdims=False)
                    pieces.append((piece * gain[None, :]).astype(jnp.bfloat16))
            for mask, piece in zip(masks, pieces):
                got[mask] = swap(piece, "tp", mask)
        return [got[mask] for mask in range(slabs)]

    first_groups, groups = piece_groups(slabs)
    gate_pieces = deliver(gate_master, norm_gain, first_groups)

    first_prob = jax.nn.sigmoid(route_logits[:, 0] - route_logits[:, 1])
    choice_prob = jnp.stack([first_prob, 1.0 - first_prob], axis=1)
    expert_ids = jnp.arange(experts, dtype=jnp.int32)
    matches = (routes[:, :, None] == expert_ids[None, None, :]).astype(jnp.float32)
    chosen = jnp.sum(matches, axis=1)
    weight = jnp.sum(matches * choice_prob[:, :, None], axis=1)
    position = jnp.cumsum(chosen, axis=0) - 1.0
    slot_ids = jnp.arange(capacity, dtype=jnp.float32)
    placed = chosen.T[:, None, :] * (position.T[:, None, :] == slot_ids[None, :, None]).astype(
        jnp.float32
    )
    placed = placed.astype(jnp.bfloat16)
    by_slab = placed.reshape(slabs, half_cap, tok_rows)
    spread = [
        jnp.concatenate(
            [
                lax.dynamic_index_in_dim(by_slab, me ^ m, 0, False)
                for m in ((2 * p + 1, 2 * p) if p else (0, 1))
            ]
        )
        for p in range(experts)
    ]
    share = [lax.dynamic_index_in_dim(weight, (me // 2) ^ p, 1) for p in range(experts)]
    picked = jnp.dot(
        placed.reshape(experts * capacity, tok_rows), tokens, preferred_element_type=jnp.float32
    )
    picked = picked.astype(jnp.bfloat16).reshape(slabs, half_cap, tokens.shape[1])
    picked, spread, share = lax.optimization_barrier((picked, spread, share))
    chunks = [
        swap(lax.dynamic_index_in_dim(picked, me ^ m, 0, keepdims=False), "tp", m)
        for m in range(slabs)
    ]
    normed = norm_rows(me_ref, chunks)
    direct = blocks <= 8
    if direct:
        gathered = [swap(normed, "fs", z) for z in range(blocks)]
        mine = jnp.concatenate(gathered, axis=0)
    else:
        mine = lax.all_gather(normed, "fs", axis=0, tiled=True)
    theirs = swap(mine, "tp", 1)

    up_pieces = deliver(up_master, norm_gain, groups)
    (masks,) = groups
    made = dict(zip(masks, ready(down_master, None, me_ref, masks)))
    down_pieces = [swap(made[mask], "tp", mask) for mask in range(slabs)]

    gate_serve, act = slab_call(gate_kernel, me_ref, (mine, theirs), None, gate_pieces, jnp.float32)
    up_serve, hidden = slab_call(up_kernel, me_ref, (mine, theirs), act, up_pieces, jnp.bfloat16)
    other_hidden = swap(hidden, "tp", 1)
    backs = {}
    down_serve = None
    for number, group in enumerate(pair_groups(experts)):
        if number == 0:
            own_pieces, other_pieces = [down_pieces[0]], [made[1]]
        else:
            own_pieces = [down_pieces[2 * pair + 1] for pair in group]
            other_pieces = [swap(down_pieces[2 * pair], "tp", 1) for pair in group]
        parts = dots_call(hidden, other_hidden, own_pieces, other_pieces, blocks)
        if direct:
            parts = [swap(part, "fs", z) for z, part in enumerate(parts)]
        else:
            parts = lax.all_to_all(jnp.stack(parts), "fs", split_axis=0, concat_axis=0, tiled=True)
        for k, pair in enumerate(group):
            total = sum(parts[z][k].astype(jnp.float32) for z in range(blocks))
            total = total.astype(jnp.bfloat16)
            backs[pair] = swap(total, "tp", 2 * pair + 1) if pair else total
        if number > 0:
            masks = [mask for pair in group for mask in (2 * pair, 2 * pair + 1)]
            filled = masks if number > 1 else [0, 1] + masks
            pieces = [down_pieces[m] for m in filled]
            model = down_pieces[0].shape[1] * slabs
            down_serve = fill_call(me_ref, pieces, filled, model, down_serve)

    mixed = jnp.zeros((tok_rows, tokens.shape[1]), jnp.float32)
    for pair in reversed(range(experts)):
        term = lax.dot_general(
            spread[pair], backs[pair], (((0,), (0,)), ((), ())), preferred_element_type=jnp.float32
        )
        mixed = mixed + share[pair] * term

    return (gate_serve, up_serve, down_serve, mixed.astype(jnp.bfloat16))


def piece_groups(slabs):
    order = [mask for mask in (4, 2, 5, 3, 6, 7, *range(8, slabs)) if mask < slabs] + [1, 0]
    return [order[:2], order[2:]], [order]


def pair_groups(experts):
    return [[0], [*range(1, experts - 1)], [experts - 1]]


def solution(mesh):
    placed = (
        P("fs", "tp"),
        P("tp"),
        P(None, "fs", "tp"),
        P(None, "fs", "tp"),
        P(None, "fs", "tp"),
        P("fs", None),
        P("fs", None),
    )
    return jax.shard_map(
        local,
        mesh=mesh,
        in_specs=placed,
        out_specs=(P("tp", "fs", None), P("tp", "fs", None), P("tp", "fs", None), P("fs", "tp")),
        check_vma=False,
    )
```

```python
import functools

import jax
import jax.numpy as jnp
from jax import lax
from jax.experimental import pallas as pl
from jax.experimental.pallas import tpu as pltpu
from jax.sharding import PartitionSpec as P


epsilon = 1e-05


def swap(value, axis, mask):
    if mask == 0:
        return value
    pairs = [(source, source ^ mask) for source in range(lax.axis_size(axis))]
    return lax.ppermute(value, axis, pairs)


def row_tile(rows):
    return rows // 2 if rows > 256 and rows % 32 == 0 else rows


def norm_kernel(me_ref, *refs):
    chunks, out_ref = refs[:-1], refs[-1]
    width = chunks[0].shape[1]
    total = jnp.zeros((chunks[0].shape[0], 1), jnp.float32)
    for ref in chunks:
        wide = ref[...].astype(jnp.float32)
        total = total + jnp.sum(wide * wide, axis=1, keepdims=True)
    scale = lax.rsqrt(total / (width * len(chunks)) + epsilon)
    for mask, ref in enumerate(chunks):
        start = pl.multiple_of((me_ref[0] ^ mask) * width, width)
        out_ref[:, pl.ds(start, width)] = (ref[...].astype(jnp.float32) * scale).astype(
            jnp.bfloat16
        )


def norm_rows(me, chunks):
    rows, width = chunks[0].shape
    return pl.pallas_call(
        norm_kernel,
        out_shape=jax.ShapeDtypeStruct((rows, width * len(chunks)), jnp.bfloat16),
        in_specs=[pl.BlockSpec(memory_space=pltpu.SMEM)]
        + [pl.BlockSpec(memory_space=pltpu.VMEM)] * len(chunks),
        out_specs=pl.BlockSpec(memory_space=pltpu.VMEM),
        cost_estimate=pl.CostEstimate(flops=10**8, bytes_accessed=10**6, transcendentals=0),
        name="norm_rows",
    )(me, *chunks)


def ready_kernel(masks, me_ref, master_ref, *refs):
    count = len(masks)
    outs, held, arrived = refs[-count - 2 : -2], refs[-2], refs[-1]
    gain = refs[0][...] if len(refs) > count + 2 else None
    copies = [
        pltpu.make_async_copy(master_ref.at[me_ref[0] ^ mask], held.at[k], arrived.at[k])
        for k, mask in enumerate(masks)
    ]
    for copy in copies:
        copy.start()
    for k, copy in enumerate(copies):
        copy.wait()
        piece = held[k] if gain is None else held[k] * gain
        outs[k][...] = piece.astype(jnp.bfloat16)


def ready(master, gain, me, masks):
    _, rows, width = master.shape
    count = len(masks)
    in_specs = [pl.BlockSpec(memory_space=pltpu.SMEM), pl.BlockSpec(memory_space=pltpu.HBM)]
    inputs = [me, master]
    if gain is not None:
        in_specs.append(pl.BlockSpec(memory_space=pltpu.VMEM))
        inputs.append(gain[None, :])
    return pl.pallas_call(
        functools.partial(ready_kernel, masks),
        in_specs=in_specs,
        out_specs=[pl.BlockSpec(memory_space=pltpu.VMEM)] * count,
        out_shape=[jax.ShapeDtypeStruct((rows, width), jnp.bfloat16)] * count,
        scratch_shapes=[
            pltpu.VMEM((count, rows, width), jnp.float32),
            pltpu.SemaphoreType.DMA((count,)),
        ],
        compiler_params=pltpu.CompilerParams(vmem_limit_bytes=57 * 2**20),
        cost_estimate=pl.CostEstimate(
            flops=10**8, bytes_accessed=6 * count * rows * width, transcendentals=0
        ),
    )(*inputs)


contract = (((1,), (1,)), ((), ()))


def place(me_ref, pieces, slab_ref):
    width = pieces[0].shape[1]
    for mask, ref in enumerate(pieces):
        start = pl.multiple_of((me_ref[0] ^ mask) * width, width)
        slab_ref[0, :, pl.ds(start, width)] = ref[...]


def gate_kernel(count, me_ref, mine_ref, theirs_ref, *refs):
    pieces, (slab_ref, act_ref) = refs[:count], refs[count:]
    place(me_ref, pieces, slab_ref)
    half = mine_ref.shape[0]
    for number, rows in enumerate((mine_ref, theirs_ref)):
        pre = lax.dot_general(rows[...], slab_ref[0], contract, preferred_element_type=jnp.float32)
        act_ref[0, pl.ds(number * half, half), :] = pre * (1.0 / (1.0 + jnp.exp(-pre)))


def up_kernel(count, me_ref, mine_ref, theirs_ref, act_ref, *refs):
    pieces, (slab_ref, hidden_ref) = refs[:count], refs[count:]
    place(me_ref, pieces, slab_ref)
    half = mine_ref.shape[0]
    for number, rows in enumerate((mine_ref, theirs_ref)):
        part = pl.ds(number * half, half)
        pre = lax.dot_general(rows[...], slab_ref[0], contract, preferred_element_type=jnp.float32)
        hidden_ref[0, part, :] = (act_ref[0, part, :] * pre).astype(jnp.bfloat16)


def fill_kernel(masks, me_ref, *refs):
    count = len(masks)
    pieces, slab_ref, left = refs[:count], refs[-2], refs[-1]
    width = pieces[0].shape[1]
    copies = []
    for k, mask in enumerate(masks):
        start = pl.multiple_of((me_ref[0] ^ mask) * width, width)
        copies.append(
            pltpu.make_async_copy(pieces[k], slab_ref.at[0, :, pl.ds(start, width)], left.at[k])
        )
    for copy in copies:
        copy.start()
    for copy in copies:
        copy.wait()


def fill_call(me, pieces, masks, model, slab):
    rows, width = pieces[0].shape
    count = len(masks)
    in_specs = [pl.BlockSpec(memory_space=pltpu.SMEM)]
    in_specs += [pl.BlockSpec(memory_space=pltpu.VMEM)] * count
    inputs = [me, *pieces]
    if slab is not None:
        in_specs.append(pl.BlockSpec(memory_space=pl.ANY))
        inputs.append(slab)
    return pl.pallas_call(
        functools.partial(fill_kernel, masks),
        in_specs=in_specs,
        out_specs=pl.BlockSpec(memory_space=pl.ANY),
        out_shape=jax.ShapeDtypeStruct((1, rows, model), jnp.bfloat16),
        input_output_aliases={} if slab is None else {1 + count: 0},
        scratch_shapes=[pltpu.SemaphoreType.DMA((count,))],
        compiler_params=pltpu.CompilerParams(vmem_limit_bytes=16 * 2**20),
        cost_estimate=pl.CostEstimate(
            flops=10**8, bytes_accessed=4 * count * rows * width, transcendentals=0
        ),
    )(*inputs)


def slab_call(kernel, me, wide, act, pieces, out_type):
    block_rows, width = pieces[0].shape
    model = width * len(pieces)
    tile = row_tile(block_rows)
    rows = sum(value.shape[0] for value in wide)
    in_specs = [pl.BlockSpec(value.shape, lambda t, me: (0, 0)) for value in wide]
    if act is not None:
        in_specs.append(pl.BlockSpec((1, rows, tile), lambda t, me: (t, 0, 0)))
    in_specs += [pl.BlockSpec((tile, width), lambda t, me: (t, 0))] * len(pieces)
    out_specs = [pl.BlockSpec((1, tile, model), lambda t, me: (0, t, 0))]
    out_shape = [jax.ShapeDtypeStruct((1, block_rows, model), jnp.bfloat16)]
    if out_type is not None:
        out_specs.append(pl.BlockSpec((1, rows, tile), lambda t, me: (t, 0, 0)))
        out_shape.append(jax.ShapeDtypeStruct((block_rows // tile, rows, tile), out_type))
    return pl.pallas_call(
        functools.partial(kernel, len(pieces)),
        grid_spec=pltpu.PrefetchScalarGridSpec(
            num_scalar_prefetch=1,
            grid=(block_rows // tile,),
            in_specs=in_specs,
            out_specs=out_specs,
        ),
        out_shape=out_shape,
        compiler_params=pltpu.CompilerParams(vmem_limit_bytes=24 * 2**20),
        cost_estimate=pl.CostEstimate(
            flops=2 * rows * block_rows * model + 10**8,
            bytes_accessed=4 * block_rows * model,
            transcendentals=0,
        ),
    )(me, *wide, *(() if act is None else (act,)), *pieces)


def dots_kernel(blocks, own_ref, other_ref, *refs):
    outs = refs[-blocks:]
    count = (len(refs) - blocks) // 2
    tiles, rows, tile = own_ref.shape
    half = rows // 2
    for number in range(count):
        own_piece, other_piece = refs[number], refs[count + number]
        for side in range(2):
            here, there = side * half, (1 - side) * half
            total = sum(
                jnp.dot(
                    hidden[t, start : start + half],
                    piece[t * tile : (t + 1) * tile],
                    preferred_element_type=jnp.float32,
                )
                for hidden, start, piece in ((own_ref, here, own_piece), (other_ref, there, other_piece))
                for t in range(tiles)
            )
            total = total.astype(jnp.bfloat16).reshape(blocks, half // blocks, -1)
            size = half // blocks
            for z in range(blocks):
                outs[z][number, side * size : (side + 1) * size] = total[z]


def base_kernel(other_ref, piece_ref, out_ref):
    tiles, rows, tile = other_ref.shape
    half = rows // 2
    for side in range(2):
        start = (1 - side) * half
        out_ref[side * half : (side + 1) * half] = sum(
            jnp.dot(
                other_ref[t, start : start + half],
                piece_ref[t * tile : (t + 1) * tile],
                preferred_element_type=jnp.float32,
            )
            for t in range(tiles)
        )


def base_call(other, piece):
    rows, (inner, width) = other.shape[1], piece.shape
    return pl.pallas_call(
        base_kernel,
        in_specs=[pl.BlockSpec(memory_space=pltpu.VMEM)] * 2,
        out_specs=pl.BlockSpec(memory_space=pltpu.VMEM),
        out_shape=jax.ShapeDtypeStruct((rows, width), jnp.float32),
        compiler_params=pltpu.CompilerParams(vmem_limit_bytes=16 * 2**20),
        cost_estimate=pl.CostEstimate(
            flops=2 * rows * inner * width + 10**8,
            bytes_accessed=2 * inner * width,
            transcendentals=0,
        ),
        name="base",
    )(other, piece)


def last_kernel(blocks, own_ref, base_ref, piece_ref, *outs):
    tiles, rows, tile = own_ref.shape
    half = rows // 2
    size = half // blocks
    for side in range(2):
        part = slice(side * half, (side + 1) * half)
        total = base_ref[part] + sum(
            jnp.dot(
                own_ref[t, part],
                piece_ref[t * tile : (t + 1) * tile],
                preferred_element_type=jnp.float32,
            )
            for t in range(tiles)
        )
        total = total.astype(jnp.bfloat16).reshape(blocks, size, -1)
        for z in range(blocks):
            outs[z][0, side * size : (side + 1) * size] = total[z]


def last_call(own, base, piece, blocks):
    rows, (inner, width) = own.shape[1], piece.shape
    out = jax.ShapeDtypeStruct((1, rows // blocks, width), jnp.bfloat16)
    return pl.pallas_call(
        functools.partial(last_kernel, blocks),
        in_specs=[pl.BlockSpec(memory_space=pltpu.VMEM)] * 3,
        out_specs=[pl.BlockSpec(memory_space=pltpu.VMEM)] * blocks,
        out_shape=[out] * blocks,
        compiler_params=pltpu.CompilerParams(vmem_limit_bytes=16 * 2**20),
        cost_estimate=pl.CostEstimate(
            flops=2 * rows * inner * width + 10**8,
            bytes_accessed=2 * inner * width,
            transcendentals=0,
        ),
    )(own, base, piece)


def dots_call(own, other, own_pieces, other_pieces, blocks):
    rows = own.shape[1]
    inner, width = own_pieces[0].shape
    count = len(own_pieces)
    out = jax.ShapeDtypeStruct((count, rows // blocks, width), jnp.bfloat16)
    return pl.pallas_call(
        functools.partial(dots_kernel, blocks),
        in_specs=[pl.BlockSpec(memory_space=pltpu.VMEM)] * (2 + 2 * count),
        out_specs=[pl.BlockSpec(memory_space=pltpu.VMEM)] * blocks,
        out_shape=[out] * blocks,
        compiler_params=pltpu.CompilerParams(vmem_limit_bytes=16 * 2**20),
        cost_estimate=pl.CostEstimate(
            flops=4 * rows * inner * width * count + 10**8,
            bytes_accessed=4 * inner * width * count,
            transcendentals=0,
        ),
    )(own, other, *own_pieces, *other_pieces)


def local(tokens, norm_gain, gate_master, up_master, down_master, routes, route_logits):
    tok_rows = tokens.shape[0]
    slabs = lax.axis_size("tp")
    blocks = lax.axis_size("fs")
    experts = slabs // 2
    capacity = tok_rows * routes.shape[1] // experts
    half_cap = capacity // 2
    me = lax.axis_index("tp")
    me_ref = me.astype(jnp.int32)[None]

    def deliver(master, gain, groups):
        got = {}
        for masks in groups:
            if len(masks) > 2:
                pieces = ready(master, gain, me_ref, masks)
            else:
                pieces = []
                for mask in masks:
                    piece = lax.dynamic_index_in_dim(master, me ^ mask, 0, keepdims=False)
                    pieces.append((piece * gain[None, :]).astype(jnp.bfloat16))
            for mask, piece in zip(masks, pieces):
                got[mask] = swap(piece, "tp", mask)
        return [got[mask] for mask in range(slabs)]

    first_groups, groups = piece_groups(slabs)
    gate_pieces = deliver(gate_master, norm_gain, first_groups)

    first_prob = jax.nn.sigmoid(route_logits[:, 0] - route_logits[:, 1])
    choice_prob = jnp.stack([first_prob, 1.0 - first_prob], axis=1)
    expert_ids = jnp.arange(experts, dtype=jnp.int32)
    matches = (routes[:, :, None] == expert_ids[None, None, :]).astype(jnp.float32)
    chosen = jnp.sum(matches, axis=1)
    weight = jnp.sum(matches * choice_prob[:, :, None], axis=1)
    position = jnp.cumsum(chosen, axis=0) - 1.0
    slot_ids = jnp.arange(capacity, dtype=jnp.float32)
    placed = chosen.T[:, None, :] * (position.T[:, None, :] == slot_ids[None, :, None]).astype(
        jnp.float32
    )
    placed = placed.astype(jnp.bfloat16)
    by_slab = placed.reshape(slabs, half_cap, tok_rows)
    spread = [
        jnp.concatenate(
            [
                lax.dynamic_index_in_dim(by_slab, me ^ m, 0, False)
                for m in ((2 * p + 1, 2 * p) if p else (0, 1))
            ]
        )
        for p in range(experts)
    ]
    share = [lax.dynamic_index_in_dim(weight, (me // 2) ^ p, 1) for p in range(experts)]
    picked = jnp.dot(
        placed.reshape(experts * capacity, tok_rows), tokens, preferred_element_type=jnp.float32
    )
    picked = picked.astype(jnp.bfloat16).reshape(slabs, half_cap, tokens.shape[1])
    picked, spread, share = lax.optimization_barrier((picked, spread, share))
    chunks = [
        swap(lax.dynamic_index_in_dim(picked, me ^ m, 0, keepdims=False), "tp", m)
        for m in range(slabs)
    ]
    normed = norm_rows(me_ref, chunks)
    direct = blocks <= 8
    if direct:
        gathered = [swap(normed, "fs", z) for z in range(blocks)]
        mine = jnp.concatenate(gathered, axis=0)
    else:
        mine = lax.all_gather(normed, "fs", axis=0, tiled=True)
    theirs = swap(mine, "tp", 1)

    up_pieces = deliver(up_master, norm_gain, groups)
    (masks,) = groups
    made = dict(zip(masks, ready(down_master, None, me_ref, masks)))
    down_pieces = [swap(made[mask], "tp", mask) for mask in range(slabs)]

    gate_serve, act = slab_call(gate_kernel, me_ref, (mine, theirs), None, gate_pieces, jnp.float32)
    up_serve, hidden = slab_call(up_kernel, me_ref, (mine, theirs), act, up_pieces, jnp.bfloat16)
    other_hidden = swap(hidden, "tp", 1)
    backs = {}
    down_serve = None
    for number, group in enumerate(pair_groups(experts)):
        if number == 0:
            own_pieces, other_pieces = [down_pieces[0]], [made[1]]
        else:
            own_pieces = [down_pieces[2 * pair + 1] for pair in group]
            other_pieces = [swap(down_pieces[2 * pair], "tp", 1) for pair in group]
        if number == 2:
            base = base_call(other_hidden, other_pieces[0])
            parts = last_call(hidden, base, own_pieces[0], blocks)
        else:
            parts = dots_call(hidden, other_hidden, own_pieces, other_pieces, blocks)
        if direct:
            parts = [swap(part, "fs", z) for z, part in enumerate(parts)]
        else:
            parts = lax.all_to_all(jnp.stack(parts), "fs", split_axis=0, concat_axis=0, tiled=True)
        for k, pair in enumerate(group):
            total = sum(parts[z][k].astype(jnp.float32) for z in range(blocks))
            total = total.astype(jnp.bfloat16)
            backs[pair] = swap(total, "tp", 2 * pair + 1) if pair else total
        if number > 0:
            masks = [mask for pair in group for mask in (2 * pair, 2 * pair + 1)]
            filled = masks if number > 1 else [0, 1] + masks
            pieces = [down_pieces[m] for m in filled]
            model = down_pieces[0].shape[1] * slabs
            down_serve = fill_call(me_ref, pieces, filled, model, down_serve)

    mixed = jnp.zeros((tok_rows, tokens.shape[1]), jnp.float32)
    for pair in reversed(range(experts)):
        term = lax.dot_general(
            spread[pair], backs[pair], (((0,), (0,)), ((), ())), preferred_element_type=jnp.float32
        )
        mixed = mixed + share[pair] * term

    return (gate_serve, up_serve, down_serve, mixed.astype(jnp.bfloat16))


def piece_groups(slabs):
    order = [mask for mask in (4, 2, 5, 3, 6, 7, *range(8, slabs)) if mask < slabs] + [1, 0]
    return [order[:2], order[2:]], [order]


def pair_groups(experts):
    return [[0], [*range(1, experts - 1)], [experts - 1]]


def solution(mesh):
    placed = (
        P("fs", "tp"),
        P("tp"),
        P(None, "fs", "tp"),
        P(None, "fs", "tp"),
        P(None, "fs", "tp"),
        P("fs", None),
        P("fs", None),
    )
    return jax.shard_map(
        local,
        mesh=mesh,
        in_specs=placed,
        out_specs=(P("tp", "fs", None), P("tp", "fs", None), P("tp", "fs", None), P("fs", "tp")),
        check_vma=False,
    )
```
